32 devices in a mesh: sp: 8 (over z, x), tp: 4 (over y, core).
Axes of the slice: x: 2, y: 2, z: 4, core: 2. Of those that a mesh axis runs over, the one named last changes fastest.
Arguments:
- residual: bfloat16 [4096, 2048], P('sp'), may hold values from -6 to 6
- queries: bfloat16 [4096, 1024], P('sp', 'tp'), may hold values from -384 to 384
- key_pairs: bfloat16 [4096, 1024], P('sp', 'tp'), may hold values from -384 to 384
- values: bfloat16 [4096, 1024], P('sp', 'tp'), may hold values from -6 to 6
- lambdas: float32 [8], P('tp'), may hold values from 0.3 to 0.8
- head_gain: float32 [128], replicated, may hold values from 0.1 to 1.9
- w_out: bfloat16 [1024, 2048], replicated, may hold values from -0.1875 to 0.1875
- norm_gain: float32 [2048], replicated, may hold values from 0.1 to 1.9
- w_gate: bfloat16 [2048, 5632], P('sp', 'tp'), may hold values from -0.125 to 0.125
- w_up: bfloat16 [2048, 5632], P('sp', 'tp'), may hold values from -0.125 to 0.125
- w_down: bfloat16 [5632, 2048], P('tp', 'sp'), may hold values from -0.078125 to 0.078125
Outputs:
- layer_out: bfloat16 [4096, 2048], P(('sp', 'tp'))
The draws below stay inside these ranges and needn't reach their ends.
All inputs are finite; a program needn't handle non-finite values.
Results may differ from the reference program's by a relative error of at most 0.018.
Values may be sent and summed in bfloat16 or wider, within the bound.
No kernel may reach another device: no remote copies, remote signals or barrier semaphores. Data moves between devices by JAX's collectives and lax.ppermute only.
A program may use at most 128 MiB of HBM per device.

```python
import math
import jax
import jax.numpy as jnp
from jax import lax

D = 2048
HEADS = 8
HD = 64
VD = 128
FF = 5632
SEQ = 4096
N_TP = 4


def drawn_pair(key):
    query_key, pair_key = jax.random.split(jax.random.fold_in(key, 11), 2)
    query_draw = jnp.clip(jax.random.normal(query_key, (SEQ, HEADS, 2, HD), jnp.float32), -6.0, 6.0) * 1.3
    key_draw = jnp.clip(jax.random.normal(pair_key, (SEQ, HEADS, 2, HD), jnp.float32), -6.0, 6.0) * 1.3
    return (query_draw.reshape(SEQ, HEADS * 2 * HD), key_draw.reshape(SEQ, HEADS * 2 * HD))


def draw_queries(key, part):
    return drawn_pair(key)[0].astype(jnp.bfloat16)


def draw_key_pairs(key, part):
    return drawn_pair(key)[1].astype(jnp.bfloat16)


def shard_levels(rng, dims, cuts, low, top_value):
    def one(position, blocks):
        draws = jax.random.uniform(jax.random.fold_in(jax.random.fold_in(rng, 6), position), (blocks,), jnp.float32, low / len(cuts), top_value / len(cuts))
        return jnp.repeat(jnp.exp(draws), dims[position] // blocks).reshape((-1,) + (1,) * (len(dims) - position - 1))

    factor_of = one(*cuts[0])
    for cut in cuts[1:]:
        factor_of = factor_of * one(*cut)
    return factor_of


def scatter_about(own_key, shape, deviation, bound, cuts=(), kind=jnp.bfloat16):
    loudness = shard_levels(own_key, shape, cuts, -0.22, 0.18) if cuts else 1.0
    result = jax.random.normal(own_key, shape, jnp.float32) * deviation * loudness
    return jnp.minimum(jnp.maximum(result, -bound), bound).astype(kind)


def setup_inputs(seed: int = 0) -> dict:
    arg_keys = jax.random.split(jax.random.key(seed), 12)
    residual = scatter_about(arg_keys[0], (SEQ, D), 1.0, 6.0, ((0, 8),))
    queries = draw_queries(jax.random.fold_in(arg_keys[11], 71), 0)
    key_pairs = draw_key_pairs(jax.random.fold_in(arg_keys[11], 71), 0)
    values = scatter_about(arg_keys[3], (SEQ, HEADS * VD), 1.0, 6.0, ((0, 8), (1, 4)))
    lambdas = jnp.clip(0.3 + 0.5 * jax.random.uniform(arg_keys[4], (HEADS,), jnp.float32) ** shard_levels(arg_keys[4], (HEADS,), ((0, 4),), -0.2, 0.2), 0.3, 0.8)
    head_gain = jnp.clip(1.0 + 0.18 * jax.random.normal(arg_keys[5], (VD,), jnp.float32), 0.1, 1.9)
    w_out = scatter_about(arg_keys[6], (HEADS * VD, D), (HEADS * VD) ** -0.5, 0.1875)
    norm_gain = jnp.clip(1.0 + 0.18 * jax.random.normal(arg_keys[7], (D,), jnp.float32), 0.1, 1.9)
    w_gate = scatter_about(arg_keys[8], (D, FF), D ** -0.5, 0.125, ((0, 8), (1, 4)))
    w_up = scatter_about(arg_keys[9], (D, FF), D ** -0.5, 0.125, ((0, 8), (1, 4)))
    w_down = scatter_about(arg_keys[10], (FF, D), FF ** -0.5, 0.078125, ((0, 4), (1, 8)))
    return {"residual": residual, "queries": queries, "key_pairs": key_pairs, "values": values, "lambdas": lambdas, "head_gain": head_gain, "w_out": w_out, "norm_gain": norm_gain, "w_gate": w_gate, "w_up": w_up, "w_down": w_down}


def reference(residual, queries, key_pairs, values, lambdas, head_gain, w_out, norm_gain, w_gate, w_up, w_down):
    score_scale = HD ** (-0.5)
    value_width = 2 * HD
    key_all = key_pairs.reshape(SEQ, HEADS, 2, HD).astype(jnp.float32)
    value_all = values.reshape(SEQ, HEADS, value_width).astype(jnp.float32)
    query_rows = math.gcd(SEQ, 256)

    def attend(query_block):
        scores = jnp.einsum('qhmd,khmd->hmqk', query_block.astype(jnp.float32), key_all) * score_scale
        highest = lax.optimization_barrier(jnp.max(scores, axis=-1, keepdims=True))
        weights = jnp.exp(scores - highest)
        totals = lax.optimization_barrier(jnp.sum(weights, axis=-1))
        rounded = lax.optimization_barrier(weights.astype(jnp.bfloat16)).astype(jnp.float32)
        mixture = jnp.einsum('hmqk,khe->hmqe', rounded, value_all) / totals[..., None]
        differ = mixture[:, 0] - lambdas[:, None, None] * mixture[:, 1]
        normed_heads = differ * lax.rsqrt(lax.optimization_barrier(jnp.mean(differ * differ, axis=-1, keepdims=True)) + 1e-05) * head_gain
        return jnp.transpose(normed_heads, (1, 0, 2)).reshape(query_rows, HEADS * value_width).astype(jnp.bfloat16)
    query_blocks = queries.reshape(SEQ // query_rows, query_rows, HEADS, 2, HD)
    heads_out = lax.map(attend, query_blocks).reshape(SEQ, HEADS * value_width)
    projected = jnp.dot(heads_out, w_out, preferred_element_type=jnp.float32)
    hidden_state = (residual.astype(jnp.float32) + projected).astype(jnp.bfloat16)
    stream_f = hidden_state.astype(jnp.float32)
    normed = (stream_f * lax.rsqrt(lax.optimization_barrier(jnp.mean(stream_f * stream_f, axis=-1, keepdims=True)) + 1e-05) * norm_gain).astype(jnp.bfloat16)
    group_width = FF // N_TP
    summed = jnp.zeros((SEQ, D), jnp.float32)
    for member in range(N_TP):
        lower = member * group_width
        gate_part = jnp.dot(normed, w_gate[:, lower:lower + group_width], preferred_element_type=jnp.float32)
        up_part = jnp.dot(normed, w_up[:, lower:lower + group_width], preferred_element_type=jnp.float32)
        hidden_part = (jax.nn.silu(gate_part) * up_part).astype(jnp.bfloat16)
        partial_sum = jnp.dot(hidden_part, w_down[lower:lower + group_width], preferred_element_type=jnp.float32)
        summed = summed + lax.optimization_barrier(partial_sum.astype(jnp.bfloat16)).astype(jnp.float32)
    return (stream_f + summed).astype(jnp.bfloat16)
```

```python
import jax
import jax.numpy as jnp
from jax import lax
from jax.sharding import PartitionSpec as P

HD = 64


def per_device(
    residual, queries, key_pairs, values, lambdas, head_gain, w_out, norm_gain, w_gate, w_up, w_down
):
    n_sp = lax.axis_size("sp")
    n_tp = lax.axis_size("tp")
    n_y = n_tp // 2
    n_x = n_y
    n_z = n_sp // n_x
    sp_index = lax.axis_index("sp")
    tp_index = lax.axis_index("tp")
    z_index = sp_index // n_x
    x_index = sp_index % n_x

    def shift_z(array, step):
        pairs = [(i, ((i // n_x + step) % n_z) * n_x + i % n_x) for i in range(n_sp)]
        return lax.ppermute(array, "sp", pairs)

    def shift_x(array, step):
        pairs = [(i, (i // n_x) * n_x + (i % n_x + step) % n_x) for i in range(n_sp)]
        return lax.ppermute(array, "sp", pairs)

    def shift_y(array, step):
        pairs = [(i, ((i // 2 + step) % n_y) * 2 + i % 2) for i in range(n_tp)]
        return lax.ppermute(array, "tp", pairs)

    def swap_core(array):
        return lax.ppermute(array, "tp", [(i, i ^ 1) for i in range(n_tp)])

    def in_order(pieces, index):
        count = len(pieces)
        ordered = []
        for place in range(count):
            chosen = pieces[0]
            for step in range(1, count):
                chosen = jnp.where((index - place) % count == step, pieces[step], chosen)
            ordered.append(chosen)
        return ordered

    local_rows = queries.shape[0]
    heads_here = lambdas.shape[0]
    value_width = values.shape[1] // heads_here
    key_width = key_pairs.shape[1]
    score_scale = HD ** (-0.5)

    own_pair = jnp.concatenate([key_pairs, values], axis=1)
    z_order = sorted(range(1, n_z), key=lambda d: min(d, n_z - d))
    column = [own_pair] + [shift_z(own_pair, d) for d in z_order]
    blocks = []
    for pair in column:
        blocks.append(pair)
        for step in range(1, n_x):
            blocks.append(shift_x(pair, step))

    def spread(weight):
        units = weight.shape[0] // n_z
        cut = weight.reshape(n_z, units, weight.shape[1])

        def for_member(step):
            return lax.dynamic_index_in_dim(cut, (z_index + step) % n_z, 0, keepdims=False)

        along_z = [for_member(0)] + [shift_z(for_member(d), d) for d in range(1, n_z)]
        columns = jnp.stack(in_order(along_z, z_index), axis=0)
        along_x = [columns] + [shift_x(columns, d) for d in range(1, n_x)]
        joined = jnp.stack(in_order(along_x, x_index), axis=1)
        rows = jnp.transpose(joined, (2, 0, 1, 3)).reshape(units, n_sp * weight.shape[1])
        along_y = [rows] + [shift_y(rows, d) for d in range(1, n_y)]
        both = along_y + [swap_core(piece) for piece in along_y]
        return both

    gate_parts = spread(w_gate.T)
    up_parts = spread(w_up.T)
    down_parts = spread(w_down)

    query_view = queries.reshape(local_rows, heads_here, 2, HD)

    def update(carry, block):
        key_block = block[:, :key_width].reshape(-1, heads_here, 2, HD)
        value_block = block[:, key_width:].reshape(-1, heads_here, value_width)
        highest, totals, mixture = carry
        scores = (
            jnp.einsum("qhmd,khmd->hmqk", query_view, key_block, preferred_element_type=jnp.float32)
            * score_scale
        )
        new_high = jnp.maximum(highest, jnp.max(scores, axis=-1))
        shrink = jnp.exp(highest - new_high)
        weights = jnp.exp(scores - new_high[..., None])
        totals = totals * shrink + jnp.sum(weights, axis=-1)
        mixture = mixture * shrink[..., None] + jnp.einsum(
            "hmqk,khe->hmqe",
            weights.astype(jnp.bfloat16),
            value_block,
            preferred_element_type=jnp.float32,
        )
        return (new_high, totals, mixture)

    carry = (
        jnp.full((heads_here, 2, local_rows), -jnp.inf, jnp.float32),
        jnp.zeros((heads_here, 2, local_rows), jnp.float32),
        jnp.zeros((heads_here, 2, local_rows, value_width), jnp.float32),
    )
    for block in blocks:
        carry = update(carry, block)
    highest, totals, mixture = carry
    mixed = mixture / totals[..., None]
    differ = mixed[:, 0] - lambdas[:, None, None] * mixed[:, 1]
    normed_heads = (
        differ * lax.rsqrt(jnp.mean(differ * differ, axis=-1, keepdims=True) + 1e-05) * head_gain
    )
    heads_out = (
        jnp.transpose(normed_heads, (1, 0, 2))
        .reshape(local_rows, heads_here * value_width)
        .astype(jnp.bfloat16)
    )

    own_rows = local_rows // n_tp
    by_owner = heads_out.reshape(n_tp, own_rows, heads_here * value_width)
    arrived = []
    for step in range(n_tp):
        piece = lax.dynamic_index_in_dim(by_owner, (tp_index + step) % n_tp, 0, keepdims=False)
        if step:
            piece = lax.ppermute(piece, "tp", [(i, (i + step) % n_tp) for i in range(n_tp)])
        arrived.append(piece)
    heads_own = jnp.concatenate(in_order(arrived, tp_index), axis=1)
    projected = jnp.dot(heads_own, w_out, preferred_element_type=jnp.float32)
    residual_own = lax.dynamic_slice_in_dim(residual, tp_index * own_rows, own_rows, 0)
    hidden_own = (residual_own.astype(jnp.float32) + projected).astype(jnp.bfloat16)
    stream_f = hidden_own.astype(jnp.float32)
    scaled = stream_f * lax.rsqrt(jnp.mean(stream_f * stream_f, axis=-1, keepdims=True) + 1e-05)
    normed_own = (scaled * norm_gain).astype(jnp.bfloat16)

    rows = jnp.concatenate([normed_own] + [shift_z(normed_own, d) for d in range(1, n_z)], axis=0)

    def times_units(parts):
        return lax.dot_general(
            rows,
            jnp.concatenate(parts, axis=0),
            (((1,), (1,)), ((), ())),
            preferred_element_type=jnp.float32,
        )

    hidden_units = (jax.nn.silu(times_units(gate_parts)) * times_units(up_parts)).astype(jnp.bfloat16)
    partial = jnp.dot(
        hidden_units, jnp.concatenate(down_parts, axis=0), preferred_element_type=jnp.float32
    ).astype(jnp.bfloat16)
    ffn_out = partial[:own_rows].astype(jnp.float32)
    for step in range(1, n_z):
        back = shift_z(partial[step * own_rows : (step + 1) * own_rows], -step)
        ffn_out = ffn_out + back.astype(jnp.float32)
    return (stream_f + ffn_out).astype(jnp.bfloat16)


def solution(mesh):
    placed = (
        P("sp", None),
        P("sp", "tp"),
        P("sp", "tp"),
        P("sp", "tp"),
        P("tp"),
        P(),
        P(),
        P(),
        P("sp", "tp"),
        P("sp", "tp"),
        P("tp", "sp"),
    )
    return jax.shard_map(
        per_device, mesh=mesh, in_specs=placed, out_specs=P(("sp", "tp"), None), check_vma=False
    )
```

```python
import jax
import jax.numpy as jnp
from jax import lax
from jax.sharding import PartitionSpec as P

HD = 64


def per_device(
    residual, queries, key_pairs, values, lambdas, head_gain, w_out, norm_gain, w_gate, w_up, w_down
):
    n_sp = lax.axis_size("sp")
    n_tp = lax.axis_size("tp")
    n_y = n_tp // 2
    n_x = n_y
    n_z = n_sp // n_x
    sp_index = lax.axis_index("sp")
    tp_index = lax.axis_index("tp")
    z_index = sp_index // n_x
    x_index = sp_index % n_x

    def shift_z(array, step):
        pairs = [(i, ((i // n_x + step) % n_z) * n_x + i % n_x) for i in range(n_sp)]
        return lax.ppermute(array, "sp", pairs)

    def shift_x(array, step):
        pairs = [(i, (i // n_x) * n_x + (i % n_x + step) % n_x) for i in range(n_sp)]
        return lax.ppermute(array, "sp", pairs)

    def shift_y(array, step):
        pairs = [(i, ((i // 2 + step) % n_y) * 2 + i % 2) for i in range(n_tp)]
        return lax.ppermute(array, "tp", pairs)

    def swap_core(array):
        return lax.ppermute(array, "tp", [(i, i ^ 1) for i in range(n_tp)])

    def in_order(pieces, index):
        count = len(pieces)
        ordered = []
        for place in range(count):
            chosen = pieces[0]
            for step in range(1, count):
                chosen = jnp.where((index - place) % count == step, pieces[step], chosen)
            ordered.append(chosen)
        return ordered

    local_rows = queries.shape[0]
    heads_here = lambdas.shape[0]
    value_width = values.shape[1] // heads_here
    key_width = key_pairs.shape[1]
    score_scale = HD ** (-0.5)

    own_pair = jnp.concatenate([key_pairs, values], axis=1)
    z_order = sorted(range(1, n_z), key=lambda d: min(d, n_z - d))
    column = [own_pair] + [shift_z(own_pair, d) for d in z_order]
    around = [[shift_x(pair, step) for step in range(1, n_x)] for pair in column]
    blocks = [own_pair] + around[0] + column[1:]
    for pieces in around[1:]:
        blocks.extend(pieces)

    def along_z(weights):
        units = weights[0].shape[0] // n_z
        cuts = [weight.reshape(n_z, units, weight.shape[1]) for weight in weights]

        def for_member(step):
            picked = [
                lax.dynamic_index_in_dim(cut, (z_index + step) % n_z, 0, keepdims=False)
                for cut in cuts
            ]
            return jnp.concatenate(picked, axis=0)

        return [for_member(0)] + [shift_z(for_member(d), d) for d in range(1, n_z)]

    def whole_rows(pieces):
        columns = jnp.stack(in_order(pieces, z_index), axis=0)
        around_x = [columns] + [shift_x(columns, d) for d in range(1, n_x)]
        joined = jnp.stack(in_order(around_x, x_index), axis=1)
        units, width = pieces[0].shape
        return jnp.transpose(joined, (2, 0, 1, 3)).reshape(units, n_sp * width)

    def along_y(array):
        return [array] + [shift_y(array, d) for d in range(1, n_y)]

    def both_cores(parts):
        return jnp.concatenate(parts + [swap_core(part) for part in parts], axis=0)

    down_columns = along_y(w_down)
    gate_pieces = along_z([w_gate.T])
    up_pieces = along_z([w_up.T])
    down_pieces = along_z(down_columns)

    query_view = queries.reshape(local_rows, heads_here, 2, HD)

    def update(carry, block):
        key_block = block[:, :key_width].reshape(-1, heads_here, 2, HD)
        value_block = block[:, key_width:].reshape(-1, heads_here, value_width)
        highest, totals, mixture = carry
        scores = (
            jnp.einsum("qhmd,khmd->hmqk", query_view, key_block, preferred_element_type=jnp.float32)
            * score_scale
        )
        new_high = jnp.maximum(highest, jnp.max(scores, axis=-1))
        shrink = jnp.exp(highest - new_high)
        weights = jnp.exp(scores - new_high[..., None])
        totals = totals * shrink + jnp.sum(weights, axis=-1)
        mixture = mixture * shrink[..., None] + jnp.einsum(
            "hmqk,khe->hmqe",
            weights.astype(jnp.bfloat16),
            value_block,
            preferred_element_type=jnp.float32,
        )
        return (new_high, totals, mixture)

    carry = (
        jnp.full((heads_here, 2, local_rows), -jnp.inf, jnp.float32),
        jnp.zeros((heads_here, 2, local_rows), jnp.float32),
        jnp.zeros((heads_here, 2, local_rows, value_width), jnp.float32),
    )
    for position, block in enumerate(blocks):
        carry = update(carry, block)
        highest, totals, mixture = carry
        if position == len(blocks) - 4:
            highest, gate_pieces = lax.optimization_barrier((highest, gate_pieces))
            gate_parts = along_y(whole_rows(gate_pieces))
        if position == len(blocks) - 3:
            highest, up_pieces = lax.optimization_barrier((highest, up_pieces))
            up_rows = whole_rows(up_pieces)
        if position == len(blocks) - 1:
            totals, down_pieces = lax.optimization_barrier((totals, down_pieces))
            down_rows = whole_rows(down_pieces)
        carry = (highest, totals, mixture)
    highest, totals, mixture = carry
    mixed = mixture / totals[..., None]
    differ = mixed[:, 0] - lambdas[:, None, None] * mixed[:, 1]
    normed_heads = (
        differ * lax.rsqrt(jnp.mean(differ * differ, axis=-1, keepdims=True) + 1e-05) * head_gain
    )
    heads_out = (
        jnp.transpose(normed_heads, (1, 0, 2))
        .reshape(local_rows, heads_here * value_width)
        .astype(jnp.bfloat16)
    )

    own_rows = local_rows // n_tp
    by_owner = heads_out.reshape(n_tp, own_rows, heads_here * value_width)
    arrived = []
    for step in range(n_tp):
        piece = lax.dynamic_index_in_dim(by_owner, (tp_index + step) % n_tp, 0, keepdims=False)
        if step:
            piece = lax.ppermute(piece, "tp", [(i, (i + step) % n_tp) for i in range(n_tp)])
        arrived.append(piece)
    arrived, up_rows = lax.optimization_barrier((arrived, up_rows))
    up_parts = along_y(up_rows)
    heads_own = jnp.concatenate(in_order(arrived, tp_index), axis=1)
    projected = jnp.dot(heads_own, w_out, preferred_element_type=jnp.float32)
    residual_own = lax.dynamic_slice_in_dim(residual, tp_index * own_rows, own_rows, 0)
    hidden_own = (residual_own.astype(jnp.float32) + projected).astype(jnp.bfloat16)
    stream_f = hidden_own.astype(jnp.float32)
    scaled = stream_f * lax.rsqrt(jnp.mean(stream_f * stream_f, axis=-1, keepdims=True) + 1e-05)
    normed_own = (scaled * norm_gain).astype(jnp.bfloat16)

    gate_whole = both_cores(gate_parts)
    up_whole = both_cores(up_parts)
    down_whole = both_cores([down_rows])

    def times_units(rows, weight):
        return lax.dot_general(
            rows, weight, (((1,), (1,)), ((), ())), preferred_element_type=jnp.float32
        )

    group = own_rows // 2
    gathered = []
    for low in range(0, own_rows, group):
        mine = normed_own[low : low + group]
        gathered.append([mine] + [shift_z(mine, d) for d in range(1, n_z)])
    finished = []
    for number, pieces in enumerate(gathered):
        rows = jnp.concatenate(pieces, axis=0)
        hidden_units = (
            jax.nn.silu(times_units(rows, gate_whole)) * times_units(rows, up_whole)
        ).astype(jnp.bfloat16)
        partial = jnp.dot(hidden_units, down_whole, preferred_element_type=jnp.float32).astype(
            jnp.bfloat16
        )
        if number + 1 < len(gathered):
            partial, gathered[number + 1] = lax.optimization_barrier((partial, gathered[number + 1]))
        summed = [partial[:group]]
        for step in range(1, n_z):
            summed.append(shift_z(partial[step * group : (step + 1) * group], -step))
        finished.append(sum(piece.astype(jnp.float32) for piece in summed))
    ffn_out = jnp.concatenate(finished, axis=0)
    return (stream_f + ffn_out).astype(jnp.bfloat16)


def solution(mesh):
    placed = (
        P("sp", None),
        P("sp", "tp"),
        P("sp", "tp"),
        P("sp", "tp"),
        P("tp"),
        P(),
        P(),
        P(),
        P("sp", "tp"),
        P("sp", "tp"),
        P("tp", "sp"),
    )
    return jax.shard_map(
        per_device, mesh=mesh, in_specs=placed, out_specs=P(("sp", "tp"), None), check_vma=False
    )
```

```python
import jax
import jax.numpy as jnp
from jax import lax
from jax.sharding import PartitionSpec as P

HD = 64


def per_device(
    residual, queries, key_pairs, values, lambdas, head_gain, w_out, norm_gain, w_gate, w_up, w_down
):
    n_sp = lax.axis_size("sp")
    n_tp = lax.axis_size("tp")
    n_y = n_tp // 2
    n_x = n_y
    n_z = n_sp // n_x
    sp_index = lax.axis_index("sp")
    tp_index = lax.axis_index("tp")
    z_index = sp_index // n_x
    x_index = sp_index % n_x

    def shift_z(array, step):
        pairs = [(i, ((i // n_x + step) % n_z) * n_x + i % n_x) for i in range(n_sp)]
        return lax.ppermute(array, "sp", pairs)

    def shift_x(array, step):
        pairs = [(i, (i // n_x) * n_x + (i % n_x + step) % n_x) for i in range(n_sp)]
        return lax.ppermute(array, "sp", pairs)

    def shift_y(array, step):
        pairs = [(i, ((i // 2 + step) % n_y) * 2 + i % 2) for i in range(n_tp)]
        return lax.ppermute(array, "tp", pairs)

    def swap_core(array):
        return lax.ppermute(array, "tp", [(i, i ^ 1) for i in range(n_tp)])

    def in_order(pieces, index):
        count = len(pieces)
        ordered = []
        for place in range(count):
            chosen = pieces[0]
            for step in range(1, count):
                chosen = jnp.where((index - place) % count == step, pieces[step], chosen)
            ordered.append(chosen)
        return ordered

    local_rows = queries.shape[0]
    heads_here = lambdas.shape[0]
    value_width = values.shape[1] // heads_here
    key_width = key_pairs.shape[1]
    score_scale = HD ** (-0.5)

    own_pair = jnp.concatenate([key_pairs, values], axis=1)
    z_order = sorted(range(1, n_z), key=lambda d: min(d, n_z - d))
    column = [own_pair] + [shift_z(own_pair, d) for d in z_order]
    around = [[shift_x(pair, step) for step in range(1, n_x)] for pair in column]
    blocks = [own_pair] + around[0] + column[1:]
    for pieces in around[1:]:
        blocks.extend(pieces)

    def along_z(weights):
        units = weights[0].shape[0] // n_z
        cuts = [weight.reshape(n_z, units, weight.shape[1]) for weight in weights]

        def for_member(step):
            picked = [
                lax.dynamic_index_in_dim(cut, (z_index + step) % n_z, 0, keepdims=False)
                for cut in cuts
            ]
            return jnp.concatenate(picked, axis=0)

        return [for_member(0)] + [shift_z(for_member(d), d) for d in range(1, n_z)]

    def whole_rows(pieces):
        columns = jnp.stack(in_order(pieces, z_index), axis=0)
        around_x = [columns] + [shift_x(columns, d) for d in range(1, n_x)]
        joined = jnp.stack(in_order(around_x, x_index), axis=1)
        units, width = pieces[0].shape
        return jnp.transpose(joined, (2, 0, 1, 3)).reshape(units, n_sp * width)

    def along_y(array):
        return [array] + [shift_y(array, d) for d in range(1, n_y)]

    def both_cores(parts):
        return jnp.concatenate(parts + [swap_core(part) for part in parts], axis=0)

    down_columns = along_y(w_down)
    gate_pieces = along_z([w_gate.T])
    up_pieces = along_z([w_up.T])
    down_pieces = along_z(down_columns)

    query_view = queries.reshape(local_rows, heads_here, 2, HD)

    def update(carry, block):
        key_block = block[:, :key_width].reshape(-1, heads_here, 2, HD)
        value_block = block[:, key_width:].reshape(-1, heads_here, value_width)
        highest, totals, mixture = carry
        scores = (
            jnp.einsum("qhmd,khmd->hmqk", query_view, key_block, preferred_element_type=jnp.float32)
            * score_scale
        )
        new_high = jnp.maximum(highest, jnp.max(scores, axis=-1))
        shrink = jnp.exp(highest - new_high)
        weights = jnp.exp(scores - new_high[..., None])
        totals = totals * shrink + jnp.sum(weights, axis=-1)
        mixture = mixture * shrink[..., None] + jnp.einsum(
            "hmqk,khe->hmqe",
            weights.astype(jnp.bfloat16),
            value_block,
            preferred_element_type=jnp.float32,
        )
        return (new_high, totals, mixture)

    carry = (
        jnp.full((heads_here, 2, local_rows), -jnp.inf, jnp.float32),
        jnp.zeros((heads_here, 2, local_rows), jnp.float32),
        jnp.zeros((heads_here, 2, local_rows, value_width), jnp.float32),
    )
    for position, block in enumerate(blocks):
        carry = update(carry, block)
        highest, totals, mixture = carry
        if position == len(blocks) - 3:
            highest, gate_pieces = lax.optimization_barrier((highest, gate_pieces))
            gate_parts = along_y(whole_rows(gate_pieces))
        if position == len(blocks) - 2:
            highest, up_pieces = lax.optimization_barrier((highest, up_pieces))
            up_rows = whole_rows(up_pieces)
        if position == len(blocks) - 1:
            totals, down_pieces = lax.optimization_barrier((totals, down_pieces))
            down_rows = whole_rows(down_pieces)
        carry = (highest, totals, mixture)
    highest, totals, mixture = carry
    mixed = mixture / totals[..., None]
    differ = mixed[:, 0] - lambdas[:, None, None] * mixed[:, 1]
    normed_heads = (
        differ * lax.rsqrt(jnp.mean(differ * differ, axis=-1, keepdims=True) + 1e-05) * head_gain
    )
    heads_out = (
        jnp.transpose(normed_heads, (1, 0, 2))
        .reshape(local_rows, heads_here * value_width)
        .astype(jnp.bfloat16)
    )

    own_rows = local_rows // n_tp
    by_owner = heads_out.reshape(n_tp, own_rows, heads_here * value_width)
    arrived = []
    for step in range(n_tp):
        piece = lax.dynamic_index_in_dim(by_owner, (tp_index + step) % n_tp, 0, keepdims=False)
        if step:
            piece = lax.ppermute(piece, "tp", [(i, (i + step) % n_tp) for i in range(n_tp)])
        arrived.append(piece)
    arrived, up_rows = lax.optimization_barrier((arrived, up_rows))
    up_parts = along_y(up_rows)
    heads_own = jnp.concatenate(in_order(arrived, tp_index), axis=1)
    projected = jnp.dot(heads_own, w_out, preferred_element_type=jnp.float32)
    residual_own = lax.dynamic_slice_in_dim(residual, tp_index * own_rows, own_rows, 0)
    hidden_own = (residual_own.astype(jnp.float32) + projected).astype(jnp.bfloat16)
    stream_f = hidden_own.astype(jnp.float32)
    scaled = stream_f * lax.rsqrt(jnp.mean(stream_f * stream_f, axis=-1, keepdims=True) + 1e-05)
    normed_own = (scaled * norm_gain).astype(jnp.bfloat16)

    gate_whole = both_cores(gate_parts)
    up_whole = both_cores(up_parts)
    down_whole = both_cores([down_rows])

    def times_units(rows, weight):
        return lax.dot_general(
            rows, weight, (((1,), (1,)), ((), ())), preferred_element_type=jnp.float32
        )

    group = own_rows // 2
    gathered = []
    for low in range(0, own_rows, group):
        mine = normed_own[low : low + group]
        gathered.append([mine] + [shift_z(mine, d) for d in range(1, n_z)])
    finished = []
    for number, pieces in enumerate(gathered):
        rows = jnp.concatenate(pieces, axis=0)
        hidden_units = (
            jax.nn.silu(times_units(rows, gate_whole)) * times_units(rows, up_whole)
        ).astype(jnp.bfloat16)
        partial = jnp.dot(hidden_units, down_whole, preferred_element_type=jnp.float32).astype(
            jnp.bfloat16
        )
        if number + 1 < len(gathered):
            partial, gathered[number + 1] = lax.optimization_barrier((partial, gathered[number + 1]))
        summed = [partial[:group]]
        for step in range(1, n_z):
            summed.append(shift_z(partial[step * group : (step + 1) * group], -step))
        finished.append(sum(piece.astype(jnp.float32) for piece in summed))
    ffn_out = jnp.concatenate(finished, axis=0)
    return (stream_f + ffn_out).astype(jnp.bfloat16)


def solution(mesh):
    placed = (
        P("sp", None),
        P("sp", "tp"),
        P("sp", "tp"),
        P("sp", "tp"),
        P("tp"),
        P(),
        P(),
        P(),
        P("sp", "tp"),
        P("sp", "tp"),
        P("tp", "sp"),
    )
    return jax.shard_map(
        per_device, mesh=mesh, in_specs=placed, out_specs=P(("sp", "tp"), None), check_vma=False
    )
```
